32 devices in a mesh: sp: 16 (over z, y, core), tp: 2 (over x).
Axes of the slice: x: 2, y: 2, z: 4, core: 2. Of those that a mesh axis runs over, the one named last changes fastest.
Arguments:
- pool_input: bfloat16 [4, 128, 8192], P(None, 'tp', 'sp'), may hold values from -8 to 8
- doc_ids: int32 [8192], P('sp'), may hold values from 0 to 3, never falling along the last dimension, each value on 1 to 4096 neighbouring positions
- pool_map: bfloat16 [4, 128, 128], replicated, may hold values from -0.5 to 0.5
- pool_scale: float32 [512], replicated, may hold values from 0.1 to 1.9
- w_out: bfloat16 [512, 2048], replicated, may hold values from -0.25 to 0.25
- residual: bfloat16 [8192, 2048], P(('sp', 'tp')), may hold values from -6 to 6
- mix_gain: float32 [2048], replicated, may hold values from 0.1 to 1.9
- ffn_gain: float32 [2048], replicated, may hold values from 0.1 to 1.9
- out_gain: float32 [2048], replicated, may hold values from 0.1 to 1.9
- expert_ids: int32 [8192, 2], P(('sp', 'tp')), may hold values from 0 to 31, all different within a row; in each aligned block of 256 rows (0 to 255, 256 to 511, ...) at most 32 rows name the same one
- route_logits: float32 [8192, 2], P(('sp', 'tp')), may hold values from -6 to 6
- w_gate: bfloat16 [32, 2048, 1024], P(('sp', 'tp')), may hold values from -0.125 to 0.125
- w_up: bfloat16 [32, 2048, 1024], P(('sp', 'tp')), may hold values from -0.125 to 0.125
- w_down: bfloat16 [32, 1024, 2048], P(('sp', 'tp')), may hold values from -0.1875 to 0.1875
Outputs:
- layer_out: bfloat16 [8192, 2048], P(('sp', 'tp'))
The draws below stay inside these ranges and needn't reach their ends.
Inputs may be any that keep to these rules, and one draw needn't show every extreme that they name: `doc_ids`: document numbers never fall along the positions; no document has more than 4096 positions. `expert_ids`: each row names 2 different experts; within each aligned block of 256 rows no expert is named by more than 32 rows, a bound that some block reaches.
All inputs are finite; a program needn't handle non-finite values.
Results may differ from the reference program's by a relative error of at most 0.03.
Values may be sent and summed in bfloat16 or wider, within the bound.
A program may use at most 64 MiB of HBM per device.

```python
import math
import jax
import jax.numpy as jnp
import numpy as np
from jax import lax

D = 2048
FF = 1024
GROUPS = 4
GROUP_W = 128
TOP_K = 2
TOK_DEV = 512
POOL_W = 512
TOKENS = 8192
ROWS_DEV = 256
EXPERTS = 32
CAP = 32
DOCS = 4
DOC_MOST = 4096
DEVICES = 32


def draw_pool_input(key, part):
    noise_key = jax.random.fold_in(key, 11)
    level_key = jax.random.fold_in(key, 12)
    span_len = max(TOK_DEV // 2, 1)
    span_count = TOKENS // span_len
    noise = jax.random.normal(noise_key, (GROUPS, GROUP_W, TOKENS), jnp.float32)
    levels = jax.random.normal(level_key, (GROUPS, GROUP_W, span_count), jnp.float32)
    full = noise + jnp.repeat(levels, span_len, axis=2)
    return jnp.clip(full, -8.0, 8.0).astype(jnp.bfloat16)


def block_scale(key, extent, pieces, low, largest):
    def one(dim, parts):
        heights = jax.random.uniform(jax.random.fold_in(jax.random.fold_in(key, 6), dim), (parts,), jnp.float32, low / len(pieces), largest / len(pieces))
        return jnp.repeat(jnp.exp(heights), extent[dim] // parts).reshape((-1,) + (1,) * (len(extent) - dim - 1))

    loudness = one(*pieces[0])
    for cut in pieces[1:]:
        loudness = loudness * one(*cut)
    return loudness


def split_up(count, total, reach, lean):
    loads = [(1 << 20) // math.isqrt(rank ** lean) + 1 for rank in range(2, count + 1)]
    surplus, given = total - reach - (count - 1), [1] * (count - 1)
    while surplus > 0:
        candidates = [i for i in range(count - 1) if given[i] < reach]
        whole, remaining = sum([loads[i] for i in candidates]), surplus
        for i in candidates:
            addition = min(reach - given[i], max(1, remaining * loads[i] // whole), surplus)
            given[i] = given[i] + addition
            surplus = surplus - addition
    return np.array([reach] + given)


def uneven_parts(own_key, number_of, total, bound, lean):
    if number_of == 2:
        one = jax.random.randint(own_key, (), max(1, total - bound), min(bound, total - 1) + 1)
        return jnp.stack([one, total - one])
    tallies = jnp.asarray(split_up(number_of, total, bound, lean), jnp.int32)
    pairs = (number_of - 1) // 2
    giver, sink = tallies[1:1 + 2 * pairs:2], tallies[2:2 + 2 * pairs:2]
    room = jnp.minimum(giver - 1, bound - sink)
    passed = jax.random.randint(jax.random.fold_in(own_key, 1), (pairs,), 0, 1 << 20) % (room + 1)
    tallies = tallies.at[1:1 + 2 * pairs:2].set(giver - passed).at[2:2 + 2 * pairs:2].set(sink + passed)
    return tallies[jax.random.permutation(jax.random.fold_in(own_key, 2), number_of)]


def deal_out(rng, own, number, rows, amount, top, limit, slope):
    order = jax.random.permutation(rng, amount)
    crowded, ordinary = portions_of(amount, rows * top, limit, slope, True), portions_of(amount, rows * top, limit, slope, False)
    places = jnp.arange(amount)

    def named(sizes, rotation):
        used = int((sizes > 0).sum())
        fixed = max(1, used // 4)
        moved = fixed + (places - fixed + rotation * (used - fixed)) % max(1, amount - fixed)
        return jnp.zeros((amount,), jnp.int32).at[order[jnp.where(places < fixed, places, moved)]].set(jnp.asarray(sizes, jnp.int32))

    sizes = jnp.where(number % 4 == 0, named(crowded, number // 4), named(ordinary, number - number // 4 - 1))
    mixed = jax.random.permutation(jax.random.fold_in(own, 3), amount)
    donor, taker = mixed[0:amount // 2 * 2:2], mixed[1:amount // 2 * 2:2]
    margin = jnp.minimum(sizes[donor] - 1, limit - sizes[taker]) // 2
    margin = jnp.where((donor == order[0]) | (taker == order[0]) | (sizes[taker] == 0), 0, jnp.maximum(margin, 0))
    moved = jax.random.randint(jax.random.fold_in(own, 4), (amount // 2,), 0, 1 << 20) % (margin + 1)
    sizes = sizes.at[donor].add(-moved).at[taker].add(moved)
    members = jnp.searchsorted(jnp.cumsum(sizes), jnp.arange(rows * top), side="right").astype(jnp.int32)
    table = members.reshape(top, rows).T
    table = table[jax.random.permutation(jax.random.fold_in(own, 1), rows)]
    rotation = jax.random.randint(jax.random.fold_in(own, 2), (rows, 1), 0, top)
    return jnp.take_along_axis(table, (jnp.arange(top)[None, :] + rotation) % top, axis=1)


def portions_of(number_of, total, bound, lean, full):
    loads = [(1 << 20) // math.isqrt(rank ** lean) + 1 for rank in range(1, number_of + 1)]
    largest = bound if full else min(bound, max(-(-total // number_of), total * loads[0] // sum(loads)))
    least = 1 if total - largest >= number_of - 1 else 0
    holding, spare = [largest] + [least] * (number_of - 1), total - largest - least * (number_of - 1)
    while spare > 0:
        free = [i for i in range(1, number_of) if holding[i] < largest] or [i for i in range(1, number_of) if holding[i] < bound]
        pool, remaining = sum([loads[i] for i in free]), spare
        for i in free:
            addition = min(bound - holding[i], max(1, remaining * loads[i] // pool), spare)
            holding[i] = holding[i] + addition
            spare = spare - addition
    return np.array(holding)


def scatter_about(rng, dims, width, reach, pieces=(), kind=jnp.bfloat16):
    loudness = block_scale(rng, dims, pieces, -0.22, 0.18) if pieces else 1.0
    array = jax.random.normal(rng, dims, jnp.float32) * width * loudness
    return jnp.minimum(jnp.maximum(array, -reach), reach).astype(kind)


def setup_inputs(seed: int = 0) -> dict:
    keys = jax.random.split(jax.random.key(seed), 15)
    pool_input = draw_pool_input(jax.random.fold_in(keys[14], 71), 0)
    doc_ids = jnp.searchsorted(jnp.cumsum(uneven_parts(keys[1], DOCS, TOKENS, DOC_MOST, 2)), jnp.arange(TOKENS), side="right").astype(jnp.int32)
    pool_map = scatter_about(keys[2], (GROUPS, GROUP_W, GROUP_W), GROUP_W ** -0.5, 0.5)
    pool_scale = jnp.clip(1.0 + 0.18 * jax.random.normal(keys[3], (POOL_W,), jnp.float32), 0.1, 1.9)
    w_out = scatter_about(keys[4], (POOL_W, D), POOL_W ** -0.5, 0.25)
    residual = scatter_about(keys[5], (TOKENS, D), 1.0, 6.0, ((0, 32),))
    mix_gain = jnp.clip(1.0 + 0.18 * jax.random.normal(keys[6], (D,), jnp.float32), 0.1, 1.9)
    ffn_gain = jnp.clip(1.0 + 0.18 * jax.random.normal(keys[7], (D,), jnp.float32), 0.1, 1.9)
    out_gain = jnp.clip(1.0 + 0.18 * jax.random.normal(keys[8], (D,), jnp.float32), 0.1, 1.9)
    expert_ids_keys = jax.random.split(jax.random.fold_in(keys[9], 1), TOKENS // ROWS_DEV)
    expert_ids_turns = jax.random.permutation(jax.random.fold_in(keys[9], 3), TOKENS // ROWS_DEV)
    expert_ids = jax.vmap(lambda own, number: deal_out(jax.random.fold_in(keys[9], 2), own, number, ROWS_DEV, EXPERTS, TOP_K, CAP, 2))(expert_ids_keys, expert_ids_turns).reshape((TOKENS, TOP_K))
    route_logits = scatter_about(keys[10], (TOKENS, TOP_K), 1.5, 6.0, ((0, 32),), jnp.float32)
    w_gate = scatter_about(keys[11], (EXPERTS, D, FF), D ** -0.5, 0.125, ((0, 32),))
    w_up = scatter_about(keys[12], (EXPERTS, D, FF), D ** -0.5, 0.125, ((0, 32),))
    w_down = scatter_about(keys[13], (EXPERTS, FF, D), FF ** -0.5, 0.1875, ((0, 32),))
    return dict(pool_input=pool_input, doc_ids=doc_ids, pool_map=pool_map, pool_scale=pool_scale, w_out=w_out, residual=residual, mix_gain=mix_gain, ffn_gain=ffn_gain, out_gain=out_gain, expert_ids=expert_ids, route_logits=route_logits, w_gate=w_gate, w_up=w_up, w_down=w_down)


def rms_scale(vector):
    return lax.rsqrt(lax.optimization_barrier(jnp.mean(vector * vector, axis=-1, keepdims=True)) + 1e-06)

def reference(pool_input, doc_ids, pool_map, pool_scale, w_out, residual, mix_gain, ffn_gain, out_gain, expert_ids, route_logits, w_gate, w_up, w_down):
    total_len = doc_ids.shape[0]
    positions = jnp.arange(total_len, dtype=jnp.int32)
    resets = jnp.concatenate([jnp.ones((1,), bool), doc_ids[1:] != doc_ids[:-1]])
    starts = lax.cummax(jnp.where(resets, positions, 0), axis=0).astype(jnp.int32)
    doc_position = (positions - starts + 1).astype(jnp.int32)
    values = pool_input.astype(jnp.float32)
    prefix = jnp.cumsum(values, axis=2)
    before = jnp.concatenate([jnp.zeros(values.shape[:2] + (1,), jnp.float32), prefix[:, :, :-1]], axis=2)
    running = prefix - jnp.take(before, starts, axis=2)
    mean_list = []
    for group_idx in range(GROUPS):
        span_len = TOK_DEV * 2 ** group_idx
        shifted = jnp.pad(running[group_idx], ((0, 0), (span_len, 0)))[:, :total_len]
        counts_in = jnp.minimum(doc_position, span_len).astype(jnp.float32)
        window = running[group_idx] - jnp.where(doc_position > span_len, shifted, jnp.float32(0.0))
        mean_list.append(window / counts_in)
    window_mean = jnp.stack(mean_list)
    pool_diff = (window_mean - values).astype(jnp.bfloat16)
    mapped = jnp.einsum('gct,gcd->tgd', pool_diff.astype(jnp.float32), pool_map.astype(jnp.float32))
    mapped = (mapped.reshape(total_len, -1) * pool_scale).astype(jnp.bfloat16)
    projected = jnp.dot(mapped, w_out, preferred_element_type=jnp.float32)
    stream = (residual.astype(jnp.float32) + mix_gain * projected * rms_scale(projected)).astype(jnp.bfloat16)
    stream_back = stream.astype(jnp.float32)
    normed = (ffn_gain * stream_back * rms_scale(stream_back)).astype(jnp.bfloat16)
    route_weight = jax.nn.sigmoid(route_logits - route_logits[:, ::-1])
    flat_expert = expert_ids.reshape(-1).astype(jnp.int32)
    flat_weight = route_weight.reshape(-1)
    flat_token = (jnp.arange(flat_expert.shape[0], dtype=jnp.int32) // TOP_K).astype(jnp.int32)
    sort_order = jnp.argsort(flat_expert, stable=True).astype(jnp.int32)
    counts = jnp.bincount(flat_expert, length=EXPERTS).astype(jnp.int32)
    expert_starts = (jnp.cumsum(counts) - counts).astype(jnp.int32)
    most_rows = DEVICES * CAP
    order_padded = jnp.concatenate([sort_order, jnp.zeros((most_rows,), jnp.int32)])

    def one_expert(total_y, expert):
        picked = lax.dynamic_slice_in_dim(order_padded, expert_starts[expert], most_rows)
        live_rows = jnp.arange(most_rows, dtype=jnp.int32) < counts[expert]
        tokens = flat_token[picked]
        row_data = normed[tokens]
        gate_act = jnp.dot(row_data, w_gate[expert], preferred_element_type=jnp.float32)
        up_act = jnp.dot(row_data, w_up[expert], preferred_element_type=jnp.float32)
        hidden = (jax.nn.silu(gate_act) * up_act).astype(jnp.bfloat16)
        expert_out = jnp.dot(hidden, w_down[expert], preferred_element_type=jnp.float32).astype(jnp.bfloat16)
        weight = jnp.where(live_rows, flat_weight[picked], jnp.float32(0.0))
        return (total_y.at[tokens].add(expert_out.astype(jnp.float32) * weight[:, None]), None)
    expert_sum, _ = lax.scan(one_expert, jnp.zeros((total_len, normed.shape[1]), jnp.float32), jnp.arange(EXPERTS, dtype=jnp.int32))
    return (stream_back + out_gain * expert_sum * rms_scale(expert_sum)).astype(jnp.bfloat16)
```

```python
import functools
import jax
import jax.numpy as jnp
from jax import lax
from jax.sharding import PartitionSpec as P
from jax.experimental import pallas as pl
from jax.experimental.pallas import tpu as pltpu

MESH = pl.DeviceIdType.MESH
EPS = 1e-06


def rms_scale(vector):
    return lax.rsqrt(jnp.mean(vector * vector, axis=-1, keepdims=True) + EPS)


def mixer_kernel(
    sp_count, tp_count,
    pool_ref, doc_ref, map_ref, scale_ref, w_out_ref, residual_ref, mix_ref, ffn_ref,
    stream_ref, normed_ref,
    tail_out, tails, run_out, far, diff_out, parts,
    tail_send, tail_recv, far_send, far_recv, diff_send, diff_recv,
):
    groups, channels, length = pool_ref.shape
    rows = length // tp_count
    lines = groups * channels
    sp, tp = lax.axis_index("sp"), lax.axis_index("tp")

    barrier = pltpu.get_barrier_semaphore()
    for i in range(1, sp_count):
        pl.semaphore_signal(
            barrier, inc=1, device_id=(lax.rem(sp + i, sp_count), tp), device_id_type=MESH
        )
    for i in range(1, tp_count):
        pl.semaphore_signal(
            barrier, inc=1, device_id=(sp, lax.rem(tp + i, tp_count)), device_id_type=MESH
        )

    values = pool_ref[...].reshape(lines, length)
    doc = doc_ref[...].astype(jnp.float32)
    last_id = doc[:, length - 1 :]
    tail_mask = jnp.broadcast_to((doc == last_id).astype(jnp.bfloat16), (8, length))
    tail_sum = lax.dot_general(
        tail_mask, values, (((1,), (1,)), ((), ())), preferred_element_type=jnp.float32
    )[:1]
    tail_count = jnp.sum((doc == last_id).astype(jnp.float32), axis=1, keepdims=True)
    tail_row = jnp.concatenate(
        [
            tail_sum,
            jnp.broadcast_to(last_id, (1, 128)),
            jnp.broadcast_to(tail_count, (1, 128)),
        ],
        axis=1,
    )
    tail_out[...] = tail_row
    tails[sp] = tail_row
    pl.semaphore_wait(barrier, sp_count + tp_count - 2)
    tail_copies = []
    for i in range(1, sp_count):
        copy = pltpu.make_async_remote_copy(
            src_ref=tail_out,
            dst_ref=tails.at[sp],
            send_sem=tail_send.at[i],
            recv_sem=tail_recv.at[i],
            device_id=(lax.rem(sp + i, sp_count), tp),
            device_id_type=MESH,
        )
        copy.start()
        tail_copies.append(copy)

    doc_col = jnp.broadcast_to(doc, (128, length)).T[:, :1]
    row_at = lax.broadcasted_iota(jnp.int32, (length, length), 0)
    col_at = lax.broadcasted_iota(jnp.int32, (length, length), 1)
    same = jnp.where((row_at <= col_at) & (doc_col == doc), 1.0, 0.0)
    local_count = jnp.sum(same, axis=0, keepdims=True)
    local_run = jnp.dot(values, same.astype(jnp.bfloat16), preferred_element_type=jnp.float32)

    for copy in tail_copies:
        copy.wait()
    table = jnp.concatenate([tails[j] for j in range(sp_count)], axis=0)
    sources = lax.broadcasted_iota(jnp.int32, (sp_count, 1), 0)
    joined = jnp.where(
        (sources < sp) & (table[:, lines : lines + 1] == doc), 1.0, 0.0
    )
    running = local_run + lax.dot_general(
        table[:, :lines],
        joined,
        (((0,), (0,)), ((), ())),
        preferred_element_type=jnp.float32,
        precision=lax.Precision.HIGHEST,
    )
    position = local_count + jnp.sum(
        joined * table[:, lines + 128 : lines + 129], axis=0, keepdims=True
    )
    run_out[...] = running.astype(jnp.bfloat16).reshape(groups, channels, length)
    far_copies = []
    for g in reversed(range(groups)):
        copy = pltpu.make_async_remote_copy(
            src_ref=run_out.at[g],
            dst_ref=far.at[g],
            send_sem=far_send.at[g],
            recv_sem=far_recv.at[g],
            device_id=(lax.rem(sp + 2**g, sp_count), tp),
            device_id_type=MESH,
        )
        copy.start()
        far_copies.append(copy)
    for copy in far_copies:
        copy.wait()
    for g in range(groups):
        span = float(length * 2**g)
        at = slice(g * channels, (g + 1) * channels)
        window = running[at] - jnp.where(position > span, far[g].astype(jnp.float32), 0.0)
        diff = window / jnp.minimum(position, span) - values[at].astype(jnp.float32)
        diff = diff.astype(jnp.bfloat16)
        for q in range(tp_count):
            diff_out[q, g] = diff[:, q * rows : (q + 1) * rows]
    parts[tp] = diff_out[tp]
    diff_copies = []
    for i in range(1, tp_count):
        other = lax.rem(tp + i, tp_count)
        copy = pltpu.make_async_remote_copy(
            src_ref=diff_out.at[other],
            dst_ref=parts.at[tp],
            send_sem=diff_send.at[i],
            recv_sem=diff_recv.at[i],
            device_id=(sp, other),
            device_id_type=MESH,
        )
        copy.start()
        diff_copies.append(copy)
    for copy in diff_copies:
        copy.wait()
    mapped = []
    for g in range(groups):
        channel_rows = jnp.concatenate([parts[q, g] for q in range(tp_count)], axis=0)
        mapped.append(
            lax.dot_general(
                channel_rows,
                map_ref[g],
                (((0,), (0,)), ((), ())),
                preferred_element_type=jnp.float32,
            )
        )
    mapped = (jnp.concatenate(mapped, axis=1) * scale_ref[...]).astype(jnp.bfloat16)
    projected = jnp.dot(mapped, w_out_ref[...], preferred_element_type=jnp.float32)
    stream = (
        residual_ref[...].astype(jnp.float32) + mix_ref[...] * projected * rms_scale(projected)
    ).astype(jnp.bfloat16)
    stream_ref[...] = stream
    back = stream.astype(jnp.float32)
    normed_ref[...] = (ffn_ref[...] * back * rms_scale(back)).astype(jnp.bfloat16)


def mixer(pool_input, doc_ids, pool_map, pool_scale, w_out, residual, mix_gain, ffn_gain):
    groups, channels, length = pool_input.shape
    sp_count, tp_count = lax.axis_size("sp"), lax.axis_size("tp")
    rows = length // tp_count
    tail_width = groups * channels + 256
    vmem = pl.BlockSpec(memory_space=pltpu.VMEM)
    shape = jax.ShapeDtypeStruct(residual.shape, jnp.bfloat16)
    return pl.pallas_call(
        functools.partial(mixer_kernel, sp_count, tp_count),
        out_shape=(shape, shape),
        in_specs=[vmem] * 8,
        out_specs=(vmem, vmem),
        scratch_shapes=[
            pltpu.VMEM((1, tail_width), jnp.float32),
            pltpu.VMEM((sp_count, 1, tail_width), jnp.float32),
            pltpu.VMEM((groups, channels, length), jnp.bfloat16),
            pltpu.VMEM((groups, channels, length), jnp.bfloat16),
            pltpu.VMEM((tp_count, groups, channels, rows), jnp.bfloat16),
            pltpu.VMEM((tp_count, groups, channels, rows), jnp.bfloat16),
            pltpu.SemaphoreType.DMA((sp_count,)),
            pltpu.SemaphoreType.DMA((sp_count,)),
            pltpu.SemaphoreType.DMA((groups,)),
            pltpu.SemaphoreType.DMA((groups,)),
            pltpu.SemaphoreType.DMA((tp_count,)),
            pltpu.SemaphoreType.DMA((tp_count,)),
        ],
        compiler_params=pltpu.CompilerParams(collective_id=0, has_side_effects=True),
    )(
        pool_input,
        doc_ids.reshape(1, -1),
        pool_map,
        pool_scale.reshape(1, -1),
        w_out,
        residual,
        mix_gain.reshape(1, -1),
        ffn_gain.reshape(1, -1),
    )


def expert_rows(row_data, w_gate, w_up, w_down):
    gate_act = jnp.dot(row_data, w_gate[0], preferred_element_type=jnp.float32)
    up_act = jnp.dot(row_data, w_up[0], preferred_element_type=jnp.float32)
    hidden = (jax.nn.silu(gate_act) * up_act).astype(jnp.bfloat16)
    return jnp.dot(hidden, w_down[0], preferred_element_type=jnp.float32).astype(jnp.bfloat16)


def slots_of(expert_ids, experts, capacity):
    rows = expert_ids.shape[0]
    ids = jnp.arange(experts, dtype=jnp.int32)
    chosen = (expert_ids[:, :, None] == ids).astype(jnp.float32)
    named = jnp.sum(chosen, axis=1)
    at = jnp.arange(rows)
    earlier = (at[:, None] > at[None, :]).astype(jnp.bfloat16)
    rank = jnp.dot(earlier, named.astype(jnp.bfloat16), preferred_element_type=jnp.float32)
    return expert_ids * capacity + jnp.sum(chosen * rank[:, None, :], axis=2).astype(jnp.int32)


def local(
    pool_input, doc_ids, pool_map, pool_scale, w_out, residual, mix_gain, ffn_gain, out_gain,
    expert_ids, route_logits, w_gate, w_up, w_down,
):
    row_count, top_count = expert_ids.shape
    width = residual.shape[1]
    experts = w_gate.shape[0] * lax.axis_size("sp") * lax.axis_size("tp")
    capacity = max(2, 2 * row_count * top_count // experts)
    slots = slots_of(expert_ids, experts, capacity)
    places = jnp.arange(experts * capacity, dtype=jnp.int32)
    picked = jnp.zeros((experts * capacity, row_count), jnp.bool_)
    for k in range(top_count):
        picked = picked | (places[:, None] == slots[:, k][None, :])
    picked = picked.astype(jnp.bfloat16)
    weights = jax.nn.sigmoid(route_logits - route_logits[:, ::-1])
    mix = jnp.zeros((row_count, experts * capacity), jnp.float32)
    for k in range(top_count):
        mix = mix + jnp.where(slots[:, k : k + 1] == places[None, :], weights[:, k : k + 1], 0.0)
    mix_high = mix.astype(jnp.bfloat16)
    mix_low = (mix - mix_high.astype(jnp.float32)).astype(jnp.bfloat16)

    stream, normed = mixer(
        pool_input, doc_ids, pool_map, pool_scale, w_out, residual, mix_gain, ffn_gain
    )
    outgoing = jnp.dot(picked, normed, preferred_element_type=jnp.float32).astype(jnp.bfloat16)
    outgoing = outgoing.reshape(experts, capacity, width)
    arrived = lax.all_to_all(outgoing, ("sp", "tp"), split_axis=0, concat_axis=0, tiled=True)
    finished = expert_rows(arrived.reshape(-1, width), w_gate, w_up, w_down).reshape(arrived.shape)
    results = lax.all_to_all(
        finished, ("sp", "tp"), split_axis=0, concat_axis=0, tiled=True
    ).reshape(-1, width)
    expert_sum = jnp.dot(mix_high, results, preferred_element_type=jnp.float32)
    expert_sum = expert_sum + jnp.dot(mix_low, results, preferred_element_type=jnp.float32)
    back = stream.astype(jnp.float32)
    return (back + out_gain * expert_sum * rms_scale(expert_sum)).astype(jnp.bfloat16)


def solution(mesh):
    rows = P(("sp", "tp"), None)
    cubes = P(("sp", "tp"), None, None)
    in_specs = (
        P(None, "tp", "sp"), P("sp"), P(), P(), P(), rows, P(), P(), P(), rows, rows,
        cubes, cubes, cubes,
    )
    return jax.shard_map(local, mesh=mesh, in_specs=in_specs, out_specs=rows, check_vma=False)
```

```python
import functools
import jax
import jax.numpy as jnp
from jax import lax
from jax.sharding import PartitionSpec as P
from jax.experimental import pallas as pl
from jax.experimental.pallas import tpu as pltpu

MESH = pl.DeviceIdType.MESH
EPS = 1e-06


def rms_scale(vector):
    return lax.rsqrt(jnp.mean(vector * vector, axis=-1, keepdims=True) + EPS)


def mixer_kernel(
    sp_count, tp_count,
    pool_ref, doc_ref, map_ref, scale_ref, w_out_ref, residual_ref, mix_ref, ffn_ref,
    stream_ref, normed_ref,
    tail_out, tails, run_out, far, diff_out, parts,
    tail_send, tail_recv, far_send, far_recv, diff_send, diff_recv,
):
    groups, channels, length = pool_ref.shape
    rows = length // tp_count
    lines = groups * channels
    sp, tp = lax.axis_index("sp"), lax.axis_index("tp")

    barrier = pltpu.get_barrier_semaphore()
    for i in range(1, sp_count):
        pl.semaphore_signal(
            barrier, inc=1, device_id=(lax.rem(sp + i, sp_count), tp), device_id_type=MESH
        )
    for i in range(1, tp_count):
        pl.semaphore_signal(
            barrier, inc=1, device_id=(sp, lax.rem(tp + i, tp_count)), device_id_type=MESH
        )

    values = pool_ref[...].reshape(lines, length)
    doc = doc_ref[...].astype(jnp.float32)
    last_id = doc[:, length - 1 :]
    tail_mask = jnp.broadcast_to((doc == last_id).astype(jnp.bfloat16), (8, length))
    tail_sum = lax.dot_general(
        tail_mask, values, (((1,), (1,)), ((), ())), preferred_element_type=jnp.float32
    )[:1]
    tail_count = jnp.sum((doc == last_id).astype(jnp.float32), axis=1, keepdims=True)
    tail_row = jnp.concatenate(
        [
            tail_sum,
            jnp.broadcast_to(last_id, (1, 128)),
            jnp.broadcast_to(tail_count, (1, 128)),
        ],
        axis=1,
    )
    tail_out[...] = tail_row
    tails[sp] = tail_row
    pl.semaphore_wait(barrier, sp_count + tp_count - 2)
    tail_copies = []
    for i in range(1, sp_count):
        copy = pltpu.make_async_remote_copy(
            src_ref=tail_out,
            dst_ref=tails.at[sp],
            send_sem=tail_send.at[i],
            recv_sem=tail_recv.at[i],
            device_id=(lax.rem(sp + i, sp_count), tp),
            device_id_type=MESH,
        )
        copy.start()
        tail_copies.append(copy)

    doc_col = jnp.broadcast_to(doc, (128, length)).T[:, :1]
    row_at = lax.broadcasted_iota(jnp.int32, (length, length), 0)
    col_at = lax.broadcasted_iota(jnp.int32, (length, length), 1)
    same = jnp.where((row_at <= col_at) & (doc_col == doc), 1.0, 0.0)
    local_count = jnp.sum(same, axis=0, keepdims=True)
    local_run = jnp.dot(values, same.astype(jnp.bfloat16), preferred_element_type=jnp.float32)

    for copy in tail_copies:
        copy.wait()
    table = jnp.concatenate([tails[j] for j in range(sp_count)], axis=0)
    sources = lax.broadcasted_iota(jnp.int32, (sp_count, 1), 0)
    joined = jnp.where(
        (sources < sp) & (table[:, lines : lines + 1] == doc), 1.0, 0.0
    )
    running = local_run + lax.dot_general(
        table[:, :lines],
        joined,
        (((0,), (0,)), ((), ())),
        preferred_element_type=jnp.float32,
        precision=lax.Precision.HIGHEST,
    )
    position = local_count + jnp.sum(
        joined * table[:, lines + 128 : lines + 129], axis=0, keepdims=True
    )
    run_out[...] = running.astype(jnp.bfloat16).reshape(groups, channels, length)
    far_copies = []
    for g in reversed(range(groups)):
        copy = pltpu.make_async_remote_copy(
            src_ref=run_out.at[g],
            dst_ref=far.at[g],
            send_sem=far_send.at[g],
            recv_sem=far_recv.at[g],
            device_id=(lax.rem(sp + 2**g, sp_count), tp),
            device_id_type=MESH,
        )
        copy.start()
        far_copies.append(copy)
    for copy in far_copies:
        copy.wait()
    for g in range(groups):
        span = float(length * 2**g)
        at = slice(g * channels, (g + 1) * channels)
        window = running[at] - jnp.where(position > span, far[g].astype(jnp.float32), 0.0)
        diff = window / jnp.minimum(position, span) - values[at].astype(jnp.float32)
        diff = diff.astype(jnp.bfloat16)
        for q in range(tp_count):
            diff_out[q, g] = diff[:, q * rows : (q + 1) * rows]
    parts[tp] = diff_out[tp]
    diff_copies = []
    for i in range(1, tp_count):
        other = lax.rem(tp + i, tp_count)
        copy = pltpu.make_async_remote_copy(
            src_ref=diff_out.at[other],
            dst_ref=parts.at[tp],
            send_sem=diff_send.at[i],
            recv_sem=diff_recv.at[i],
            device_id=(sp, other),
            device_id_type=MESH,
        )
        copy.start()
        diff_copies.append(copy)
    for copy in diff_copies:
        copy.wait()
    mapped = []
    for g in range(groups):
        channel_rows = jnp.concatenate([parts[q, g] for q in range(tp_count)], axis=0)
        mapped.append(
            lax.dot_general(
                channel_rows,
                map_ref[g],
                (((0,), (0,)), ((), ())),
                preferred_element_type=jnp.float32,
            )
        )
    mapped = (jnp.concatenate(mapped, axis=1) * scale_ref[...]).astype(jnp.bfloat16)
    projected = jnp.dot(mapped, w_out_ref[...], preferred_element_type=jnp.float32)
    stream = (
        residual_ref[...].astype(jnp.float32) + mix_ref[...] * projected * rms_scale(projected)
    ).astype(jnp.bfloat16)
    stream_ref[...] = stream
    back = stream.astype(jnp.float32)
    normed_ref[...] = (ffn_ref[...] * back * rms_scale(back)).astype(jnp.bfloat16)


def mixer(pool_input, doc_ids, pool_map, pool_scale, w_out, residual, mix_gain, ffn_gain):
    groups, channels, length = pool_input.shape
    sp_count, tp_count = lax.axis_size("sp"), lax.axis_size("tp")
    rows = length // tp_count
    tail_width = groups * channels + 256
    vmem = pl.BlockSpec(memory_space=pltpu.VMEM)
    shape = jax.ShapeDtypeStruct(residual.shape, jnp.bfloat16)
    return pl.pallas_call(
        functools.partial(mixer_kernel, sp_count, tp_count),
        out_shape=(shape, shape),
        in_specs=[vmem] * 8,
        out_specs=(vmem, vmem),
        scratch_shapes=[
            pltpu.VMEM((1, tail_width), jnp.float32),
            pltpu.VMEM((sp_count, 1, tail_width), jnp.float32),
            pltpu.VMEM((groups, channels, length), jnp.bfloat16),
            pltpu.VMEM((groups, channels, length), jnp.bfloat16),
            pltpu.VMEM((tp_count, groups, channels, rows), jnp.bfloat16),
            pltpu.VMEM((tp_count, groups, channels, rows), jnp.bfloat16),
            pltpu.SemaphoreType.DMA((sp_count,)),
            pltpu.SemaphoreType.DMA((sp_count,)),
            pltpu.SemaphoreType.DMA((groups,)),
            pltpu.SemaphoreType.DMA((groups,)),
            pltpu.SemaphoreType.DMA((tp_count,)),
            pltpu.SemaphoreType.DMA((tp_count,)),
        ],
        compiler_params=pltpu.CompilerParams(collective_id=0, has_side_effects=True),
    )(
        pool_input,
        doc_ids.reshape(1, -1),
        pool_map,
        pool_scale.reshape(1, -1),
        w_out,
        residual,
        mix_gain.reshape(1, -1),
        ffn_gain.reshape(1, -1),
    )


def expert_rows(row_data, w_gate, w_up, w_down):
    gate_act = jnp.dot(row_data, w_gate[0], preferred_element_type=jnp.float32)
    up_act = jnp.dot(row_data, w_up[0], preferred_element_type=jnp.float32)
    hidden = (jax.nn.silu(gate_act) * up_act).astype(jnp.bfloat16)
    return jnp.dot(hidden, w_down[0], preferred_element_type=jnp.float32).astype(jnp.bfloat16)


def slots_of(expert_ids, experts, part):
    rows = expert_ids.shape[0]
    ids = jnp.arange(experts, dtype=jnp.int32)
    chosen = (expert_ids[:, :, None] == ids).astype(jnp.float32)
    named = jnp.sum(chosen, axis=1)
    at = jnp.arange(rows)
    earlier = (at[:, None] > at[None, :]).astype(jnp.bfloat16)
    rank = jnp.dot(earlier, named.astype(jnp.bfloat16), preferred_element_type=jnp.float32)
    rank = jnp.sum(chosen * rank[:, None, :], axis=2).astype(jnp.int32)
    piece = rank // part
    return (piece * experts + expert_ids) * part + rank - piece * part


def local(
    pool_input, doc_ids, pool_map, pool_scale, w_out, residual, mix_gain, ffn_gain, out_gain,
    expert_ids, route_logits, w_gate, w_up, w_down,
):
    row_count, top_count = expert_ids.shape
    width = residual.shape[1]
    experts = w_gate.shape[0] * lax.axis_size("sp") * lax.axis_size("tp")
    capacity = max(2, 2 * row_count * top_count // experts)
    pieces = 2 if capacity % 2 == 0 else 1
    part = capacity // pieces
    slots = slots_of(expert_ids, experts, part)
    places = jnp.arange(experts * capacity, dtype=jnp.int32)
    picked = jnp.zeros((experts * capacity, row_count), jnp.bool_)
    for k in range(top_count):
        picked = picked | (places[:, None] == slots[:, k][None, :])
    picked = picked.astype(jnp.bfloat16)
    weights = jax.nn.sigmoid(route_logits - route_logits[:, ::-1])
    mix = jnp.zeros((row_count, experts * capacity), jnp.float32)
    for k in range(top_count):
        mix = mix + jnp.where(slots[:, k : k + 1] == places[None, :], weights[:, k : k + 1], 0.0)
    mix_high = mix.astype(jnp.bfloat16)
    mix_low = (mix - mix_high.astype(jnp.float32)).astype(jnp.bfloat16)

    stream, normed = mixer(
        pool_input, doc_ids, pool_map, pool_scale, w_out, residual, mix_gain, ffn_gain
    )
    axes = ("sp", "tp")
    spans = [slice(i * experts * part, (i + 1) * experts * part) for i in range(pieces)]
    arrived = []
    for span in spans:
        outgoing = jnp.dot(picked[span], normed, preferred_element_type=jnp.float32)
        outgoing = outgoing.astype(jnp.bfloat16).reshape(experts, part, width)
        arrived.append(lax.all_to_all(outgoing, axes, split_axis=0, concat_axis=0, tiled=True))
    results = []
    for rows in arrived:
        finished = expert_rows(rows.reshape(-1, width), w_gate, w_up, w_down).reshape(rows.shape)
        results.append(lax.all_to_all(finished, axes, split_axis=0, concat_axis=0, tiled=True))
    expert_sum = jnp.zeros((row_count, width), jnp.float32)
    for span, rows in zip(spans, results):
        rows = rows.reshape(-1, width)
        for share in (mix_high, mix_low):
            expert_sum = expert_sum + jnp.dot(
                share[:, span], rows, preferred_element_type=jnp.float32
            )
    back = stream.astype(jnp.float32)
    return (back + out_gain * expert_sum * rms_scale(expert_sum)).astype(jnp.bfloat16)


def solution(mesh):
    rows = P(("sp", "tp"), None)
    cubes = P(("sp", "tp"), None, None)
    in_specs = (
        P(None, "tp", "sp"), P("sp"), P(), P(), P(), rows, P(), P(), P(), rows, rows,
        cubes, cubes, cubes,
    )
    return jax.shard_map(local, mesh=mesh, in_specs=in_specs, out_specs=rows, check_vma=False)
```
